32 devices in a mesh: sp: 16 (over z, y, core), tp: 2 (over x).
Axes of the slice: x: 2, y: 2, z: 4, core: 2. Of those that a mesh axis runs over, the one named last changes fastest.
Arguments:
- layer_source_rows: bfloat16 [6144, 2048], P(('sp', 'tp')), may hold values from -6 to 6
- entry_rescale_factor: bfloat16 [2048], replicated, may hold values from 0.099609375 to 1.8984375
- sliding_mixer_entry_matrix: bfloat16 [3, 2048, 1024], P(None, 'sp', 'tp'), may hold values from -0.125 to 0.125
- recurrent_mixer_entry_matrix: bfloat16 [2, 2048, 1024], P(None, 'sp', 'tp'), may hold values from -0.125 to 0.125
- latent_write_read_matrix: bfloat16 [2, 2048, 2048], P(None, 'sp', 'tp'), may hold values from -0.125 to 0.125
- timestep_matrix: bfloat16 [2048, 2, 16], P(None, None, 'tp'), may hold values from -0.125 to 0.125
- sliding_kernel_coefficients: bfloat16 [3, 1024], P(None, 'tp'), may hold values from -3.5 to 3.5
- recurrent_kernel_coefficients: bfloat16 [5, 1024], P(None, 'tp'), may hold values from -0.5 to 0.5
- latent_kernel_coefficients: bfloat16 [5, 2, 2048], P(None, None, 'tp'), may hold values from -0.5 to 0.5
- lane_forgetting_rate: float32 [2, 16], P(None, 'tp'), may hold values from 0 to 1
- spike_forgetting_rate: float32 [6144, 16], P('sp', 'tp'), may hold values from -2 to 0
- lane_rescale_factor: bfloat16 [1024], P('tp'), may hold values from 0.099609375 to 1.8984375
- sliding_mixer_exit_matrix: bfloat16 [1024, 2048], P('tp', 'sp'), may hold values from -0.125 to 0.125
- recurrent_mixer_exit_matrix: bfloat16 [1024, 2048], P('tp', 'sp'), may hold values from -0.125 to 0.125
Outputs:
- mixed_out: bfloat16 [6144, 2048], P(('sp', 'tp'))
The draws below stay inside these ranges and needn't reach their ends.
All inputs are finite; a program needn't handle non-finite values.
Results may differ from the reference program's by a relative error of at most 0.017.
Values may be sent and summed in bfloat16 or wider, within the bound.
A program may use at most 64 MiB of HBM per device.

```python
import jax
import jax.numpy as jnp
from jax import lax

D = 2048
CONV_CH = 1024
MIXER_LANES = 16
HEAD_DIM = 64
GROUPS = 16
STATE = 128
BLOCK = 128
CONV_TAPS = 3
SSD_TAPS = 5
TOK_DEV = 384
SSD_W = 1024
GROUP_HEADS = 1
SEQ_LENGTH = 6144
N_TP = 2


def draw_lane_forgetting_rate(key, part):
    flag_key = jax.random.fold_in(key, 11)
    level_key = jax.random.fold_in(key, 12)
    fraction = jax.random.uniform(level_key, (2, MIXER_LANES), jnp.float32)
    slow_rates = jnp.exp(jnp.log(0.1 / SEQ_LENGTH) + fraction * jnp.log(5.0))
    fast_rates = jnp.exp(jnp.log(0.01) + fraction * jnp.log(4.0))
    fast_flag = jax.random.randint(flag_key, (2, MIXER_LANES), 0, 2) == 1
    return jnp.where(fast_flag, fast_rates, slow_rates).astype(jnp.float32)


def draw_spike_forgetting_rate(key, part):
    level_key = jax.random.fold_in(key, 21)
    where_random_seed = jax.random.fold_in(key, 22)
    amount_random_seed = jax.random.fold_in(key, 23)
    blocks = SEQ_LENGTH // TOK_DEV
    fraction = jax.random.uniform(level_key, (blocks, MIXER_LANES), jnp.float32)
    levels = jnp.exp(jnp.log(0.1 / SEQ_LENGTH) + fraction * jnp.log(10.0))
    spread_amounts = jnp.repeat(levels, TOK_DEV, axis=0)
    spike_sites = jax.random.randint(where_random_seed, (3, MIXER_LANES), 0, SEQ_LENGTH)
    spike_amounts = jax.random.uniform(amount_random_seed, (3, MIXER_LANES), jnp.float32, 0.22, 0.5)
    sequence_indices = jnp.arange(SEQ_LENGTH)[:, None, None]
    spike_counts = (sequence_indices == spike_sites[None]).astype(jnp.float32)
    return (-spread_amounts - jnp.sum(spike_counts * spike_amounts[None], axis=1)).astype(jnp.float32)


def level_of(key, shape, pieces, least, high):
    loudness, own = 1.0, jax.random.fold_in(key, 6)
    for dim, shards_of in pieces:
        draws = jnp.exp(jax.random.uniform(jax.random.fold_in(own, dim), (shards_of,), jnp.float32, least / len(pieces), high / len(pieces)))
        loudness = loudness * jnp.repeat(draws, shape[dim] // shards_of).reshape([-1 if axis == dim else 1 for axis in range(len(shape))])
    return loudness


def gaussian(own_key, extent, deviation, reach, shards=(), kind=jnp.bfloat16):
    values = deviation * jax.random.normal(own_key, extent, jnp.float32)
    if shards:
        values = values * level_of(own_key, extent, shards, -0.22, 0.18)
    return jnp.clip(values, -reach, reach).astype(kind)


def setup_inputs(seed: int = 0) -> dict:
    streams_of = jax.random.split(jax.random.key(seed), 15)
    layer_source_rows = gaussian(streams_of[0], (SEQ_LENGTH, D), 1.0, 6.0, ((0, 32),))
    entry_rescale_factor = jnp.clip(1.0 + 0.18 * jax.random.normal(streams_of[1], (D,), jnp.float32), 0.099609375, 1.8984375).astype(jnp.bfloat16)
    sliding_mixer_entry_matrix = gaussian(streams_of[2], (3, D, CONV_CH), D ** -0.5, 0.125, ((1, 16), (2, 2)))
    recurrent_mixer_entry_matrix = gaussian(streams_of[3], (2, D, SSD_W), D ** -0.5, 0.125, ((1, 16), (2, 2)))
    latent_write_read_matrix = gaussian(streams_of[4], (2, D, GROUPS * STATE), D ** -0.5, 0.125, ((1, 16), (2, 2)))
    timestep_matrix = gaussian(streams_of[5], (D, 2, MIXER_LANES), D ** -0.5, 0.125, ((2, 2),))
    sliding_kernel_coefficients = gaussian(streams_of[6], (CONV_TAPS, CONV_CH), CONV_TAPS ** -0.5, 3.5, ((1, 2),))
    recurrent_kernel_coefficients = gaussian(streams_of[7], (SSD_TAPS, SSD_W), 0.09, 0.5, ((1, 2),))
    latent_kernel_coefficients = gaussian(streams_of[8], (SSD_TAPS, 2, GROUPS * STATE), 0.09, 0.5, ((2, 2),))
    lane_forgetting_rate = draw_lane_forgetting_rate(jax.random.fold_in(streams_of[14], 71), 0)
    spike_forgetting_rate = draw_spike_forgetting_rate(jax.random.fold_in(streams_of[14], 71), 0)
    lane_rescale_factor = jnp.clip(1.0 + 0.18 * jax.random.normal(streams_of[11], (SSD_W,), jnp.float32), 0.099609375, 1.8984375).astype(jnp.bfloat16)
    sliding_mixer_exit_matrix = gaussian(streams_of[12], (CONV_CH, D), (CONV_CH + SSD_W) ** -0.5, 0.125, ((0, 2), (1, 16)))
    recurrent_mixer_exit_matrix = gaussian(streams_of[13], (SSD_W, D), (CONV_CH + SSD_W) ** -0.5, 0.125, ((0, 2), (1, 16)))
    return dict(layer_source_rows=layer_source_rows, entry_rescale_factor=entry_rescale_factor, sliding_mixer_entry_matrix=sliding_mixer_entry_matrix, recurrent_mixer_entry_matrix=recurrent_mixer_entry_matrix, latent_write_read_matrix=latent_write_read_matrix, timestep_matrix=timestep_matrix, sliding_kernel_coefficients=sliding_kernel_coefficients, recurrent_kernel_coefficients=recurrent_kernel_coefficients, latent_kernel_coefficients=latent_kernel_coefficients, lane_forgetting_rate=lane_forgetting_rate, spike_forgetting_rate=spike_forgetting_rate, lane_rescale_factor=lane_rescale_factor, sliding_mixer_exit_matrix=sliding_mixer_exit_matrix, recurrent_mixer_exit_matrix=recurrent_mixer_exit_matrix)


epsilon = 1e-05

def centred_taps(values, tap_table):
    tap_count = tap_table.shape[0]
    half_width = tap_count // 2
    length = values.shape[0]
    padded = jnp.pad(values, ((half_width, half_width), (0, 0)))
    summed = jnp.zeros(values.shape, jnp.float32)
    for offset in range(tap_count):
        summed = summed + padded[offset:offset + length] * tap_table[offset].astype(jnp.float32)
    return summed

def project(normed, weight):
    return jnp.dot(normed, weight, preferred_element_type=jnp.float32).astype(jnp.bfloat16)

def direction_pass(ssd_x, keys_b, reads_c, timestep_deltas, forgetting_exponent):
    length = ssd_x.shape[0]
    blocks = length // BLOCK
    x_blocks = ssd_x.reshape(blocks, BLOCK, GROUPS, GROUP_HEADS, HEAD_DIM)
    b_blocks = keys_b.reshape(blocks, BLOCK, GROUPS, STATE)
    c_blocks = reads_c.reshape(blocks, BLOCK, GROUPS, STATE)
    d_blocks = timestep_deltas.reshape(blocks, BLOCK, GROUPS, GROUP_HEADS)
    l_blocks = forgetting_exponent.reshape(blocks, BLOCK, GROUPS, GROUP_HEADS)
    lower_mask = (jnp.arange(BLOCK)[:, None] >= jnp.arange(BLOCK)[None, :])[:, :, None, None]

    def one_block(carry_state, inputs):
        x_block, b_block, c_block, d_block, l_block = inputs
        running = jnp.cumsum(l_block, axis=0)
        log_gaps = jnp.where(lower_mask, running[:, None] - running[None, :], 0.0)
        decays = jnp.where(lower_mask, jnp.exp(log_gaps), 0.0)
        scores = jnp.einsum('tgn,sgn->tsg', c_block.astype(jnp.float32), b_block.astype(jnp.float32))
        weights = (scores[..., None] * decays * d_block[None]).astype(jnp.bfloat16)
        within = jnp.einsum('tsgr,sgrp->tgrp', weights.astype(jnp.float32), x_block.astype(jnp.float32))
        entering = lax.optimization_barrier(carry_state.astype(jnp.bfloat16)).astype(jnp.float32)
        carried = jnp.einsum('tgn,grpn->tgrp', c_block.astype(jnp.float32), entering) * jnp.exp(running)[..., None]
        to_end = jnp.exp(running[-1][None] - running) * d_block
        weighted = (x_block.astype(jnp.float32) * to_end[..., None]).astype(jnp.bfloat16)
        contribution = jnp.einsum('sgrp,sgn->grpn', weighted.astype(jnp.float32), b_block.astype(jnp.float32))
        next_state = carry_state * jnp.exp(running[-1])[..., None, None] + contribution
        return (next_state, within + carried)
    initial = jnp.zeros((GROUPS, GROUP_HEADS, HEAD_DIM, STATE), jnp.float32)
    final_state, outputs = lax.scan(one_block, initial, (x_blocks, b_blocks, c_blocks, d_blocks, l_blocks))
    return outputs.reshape(length, GROUPS, GROUP_HEADS, HEAD_DIM)

def reference(layer_source_rows, entry_rescale_factor, sliding_mixer_entry_matrix, recurrent_mixer_entry_matrix, latent_write_read_matrix, timestep_matrix, sliding_kernel_coefficients, recurrent_kernel_coefficients, latent_kernel_coefficients, lane_forgetting_rate, spike_forgetting_rate, lane_rescale_factor, sliding_mixer_exit_matrix, recurrent_mixer_exit_matrix):
    float_rows = layer_source_rows.astype(jnp.float32)
    normed = (float_rows * lax.rsqrt(lax.optimization_barrier(jnp.mean(float_rows * float_rows, axis=-1, keepdims=True)) + epsilon) * entry_rescale_factor.astype(jnp.float32)).astype(jnp.bfloat16)
    out_gate = project(normed, sliding_mixer_entry_matrix[0])
    in_gate = project(normed, sliding_mixer_entry_matrix[1])
    values = project(normed, sliding_mixer_entry_matrix[2])
    ssd_gate = project(normed, recurrent_mixer_entry_matrix[0])
    ssd_in = project(normed, recurrent_mixer_entry_matrix[1])
    inject = project(normed, latent_write_read_matrix[0])
    readout = project(normed, latent_write_read_matrix[1])
    raw_step = project(normed, timestep_matrix.reshape(timestep_matrix.shape[0], 2 * MIXER_LANES)).reshape(-1, 2, MIXER_LANES)
    gated_in = (in_gate.astype(jnp.float32) * values.astype(jnp.float32)).astype(jnp.bfloat16)
    y_conv = (out_gate.astype(jnp.float32) * centred_taps(gated_in.astype(jnp.float32), sliding_kernel_coefficients)).astype(jnp.bfloat16)
    joined = jnp.concatenate([ssd_in, inject, readout], axis=1).astype(jnp.float32)
    joined_taps = jnp.concatenate([recurrent_kernel_coefficients, latent_kernel_coefficients.reshape(latent_kernel_coefficients.shape[0], -1)], axis=1)
    mixed_ssd = jax.nn.silu(centred_taps(joined, joined_taps)).astype(jnp.bfloat16)
    length = layer_source_rows.shape[0]
    ssd_x = mixed_ssd[:, :SSD_W]
    keys_b = mixed_ssd[:, SSD_W:SSD_W + GROUPS * STATE]
    reads_c = mixed_ssd[:, SSD_W + GROUPS * STATE:]
    timestep_deltas = jax.nn.softplus(raw_step.astype(jnp.float32))
    forgetting_exponent = -timestep_deltas * lane_forgetting_rate.astype(jnp.float32)[None] + spike_forgetting_rate.astype(jnp.float32)[:, None, :]
    y_fwd = direction_pass(ssd_x, keys_b, reads_c, timestep_deltas[:, 0], forgetting_exponent[:, 0])
    y_bwd = jnp.flip(direction_pass(jnp.flip(ssd_x, 0), jnp.flip(keys_b, 0), jnp.flip(reads_c, 0), jnp.flip(timestep_deltas[:, 1], 0), jnp.flip(forgetting_exponent[:, 1], 0)), 0)
    gated_out = (y_fwd + y_bwd).reshape(length, SSD_W) * jax.nn.silu(ssd_gate.astype(jnp.float32))
    grouped = gated_out.reshape(length, GROUPS, GROUP_HEADS * HEAD_DIM)
    grouped = grouped * lax.rsqrt(lax.optimization_barrier(jnp.mean(grouped * grouped, axis=-1, keepdims=True)) + epsilon)
    y_ssd = (grouped.reshape(length, SSD_W) * lane_rescale_factor.astype(jnp.float32)).astype(jnp.bfloat16)
    conv_part = CONV_CH // N_TP
    ssd_part = SSD_W // N_TP
    summed = jnp.zeros((length, D), jnp.float32)
    for source in range(N_TP):
        partial_value = jnp.dot(y_conv[:, source * conv_part:(source + 1) * conv_part], sliding_mixer_exit_matrix[source * conv_part:(source + 1) * conv_part], preferred_element_type=jnp.float32)
        partial_value = partial_value + jnp.dot(y_ssd[:, source * ssd_part:(source + 1) * ssd_part], recurrent_mixer_exit_matrix[source * ssd_part:(source + 1) * ssd_part], preferred_element_type=jnp.float32)
        summed = summed + lax.optimization_barrier(partial_value.astype(jnp.bfloat16)).astype(jnp.float32)
    return summed.astype(jnp.bfloat16)
```

```python
import functools

import jax
import jax.numpy as jnp
from jax import lax
from jax.experimental import pallas as pl
from jax.experimental.pallas import tpu as pltpu
from jax.sharding import PartitionSpec as P

HEAD_DIM = 64
STATE = 128
HALO = 8
CHUNKS = 2
epsilon = 1e-05
F32 = jnp.float32
BF16 = jnp.bfloat16
HIGHEST = lax.Precision.HIGHEST


def ring_kernel(n, w_ref, out_ref, own_sem, ring_send, ring_recv, mate_send, mate_recv):
    chips = n // 2
    me = lax.axis_index("sp")
    core, chip = me % 2, me // 2
    odd = chip % 2
    spot = (1 - odd) * (chip // 2) + odd * (chips - 1 - chip // 2)

    def device(position):
        position = (position + 2 * chips) % chips
        half = (chips + 1) // 2
        late = position // half
        late_chip = 2 * (chips - 1 - position) + 1
        return 2 * ((1 - late) * 2 * position + late * late_chip) + core

    mate = me + 1 - 2 * core
    ways = (device(spot + 1), device(spot - 1))
    rows = w_ref.shape[0] // (2 * CHUNKS)

    barrier = pltpu.get_barrier_semaphore()
    for other in (mate,) + ways:
        pl.semaphore_signal(
            barrier, inc=1, device_id={"sp": other}, device_id_type=pl.DeviceIdType.MESH
        )
    pl.semaphore_wait(barrier, 3)

    def piece(way, chunk):
        return pl.ds((way * CHUNKS + chunk) * rows, rows)

    def ring_copy(step, way, chunk):
        owner = device(spot - step if way == 0 else spot + step)
        part = piece(way, chunk)
        return pltpu.make_async_remote_copy(
            src_ref=w_ref.at[part] if step == 0 else out_ref.at[owner, part],
            dst_ref=out_ref.at[owner, part],
            send_sem=ring_send.at[step, way, chunk],
            recv_sem=ring_recv.at[step, way, chunk],
            device_id={"sp": ways[way]},
            device_id_type=pl.DeviceIdType.MESH,
        )

    def arrival(step, way, chunk):
        owner = device(spot - step - 1 if way == 0 else spot + step + 1)
        part = piece(way, chunk)
        return pltpu.make_async_remote_copy(
            src_ref=out_ref.at[owner, part],
            dst_ref=out_ref.at[owner, part],
            send_sem=ring_send.at[step, way, chunk],
            recv_sem=ring_recv.at[step, way, chunk],
            device_id={"sp": ways[way]},
            device_id_type=pl.DeviceIdType.MESH,
        )

    def mate_copy(step, way, chunk, incoming=False):
        owner = device(spot - step if way == 0 else spot + step)
        if incoming:
            owner = owner + 1 - 2 * core
        part = piece(way, chunk)
        return pltpu.make_async_remote_copy(
            src_ref=w_ref.at[part] if step == 0 else out_ref.at[owner, part],
            dst_ref=out_ref.at[owner, part],
            send_sem=mate_send.at[step, way, chunk],
            recv_sem=mate_recv.at[step, way, chunk],
            device_id={"sp": mate},
            device_id_type=pl.DeviceIdType.MESH,
        )

    parts = [(way, chunk) for chunk in range(CHUNKS) for way in range(2)]
    for way, chunk in parts:
        ring_copy(0, way, chunk).start()
    for way, chunk in parts:
        mate_copy(0, way, chunk).start()
    own = pltpu.make_async_copy(w_ref, out_ref.at[me], own_sem)
    own.start()
    for step in range(chips - 1):
        for way, chunk in parts:
            arrival(step, way, chunk).wait_recv()
            if step < chips - 2:
                ring_copy(step + 1, way, chunk).start()
            mate_copy(step + 1, way, chunk).start()
    own.wait()
    for step in range(chips):
        for way, chunk in parts:
            if step < chips - 1:
                ring_copy(step, way, chunk).wait_send()
            mate_copy(step, way, chunk).wait_send()
            mate_copy(step, way, chunk, True).wait_recv()


def gather_rows(block):
    n = lax.axis_size("sp")
    chips = n // 2
    rows, cols = block.shape
    return pl.pallas_call(
        functools.partial(ring_kernel, n),
        out_shape=jax.ShapeDtypeStruct((n, rows, cols), block.dtype),
        in_specs=[pl.BlockSpec(memory_space=pltpu.VMEM)],
        out_specs=pl.BlockSpec(memory_space=pl.ANY),
        scratch_shapes=[
            pltpu.SemaphoreType.DMA,
            pltpu.SemaphoreType.DMA((chips - 1, 2, CHUNKS)),
            pltpu.SemaphoreType.DMA((chips - 1, 2, CHUNKS)),
            pltpu.SemaphoreType.DMA((chips, 2, CHUNKS)),
            pltpu.SemaphoreType.DMA((chips, 2, CHUNKS)),
        ],
        compiler_params=pltpu.CompilerParams(
            collective_id=0, has_side_effects=True, vmem_limit_bytes=16 * 2**20
        ),
        cost_estimate=pl.CostEstimate(
            flops=0, bytes_accessed=n * rows * cols * 16, transcendentals=0
        ),
    )(block)


def taps_of(padded, table, length):
    full = padded.shape[0]
    half = table.shape[0] // 2
    total = None
    for k in range(table.shape[0]):
        moved = padded if k == half else pltpu.roll(padded, (half - k) % full, 0)
        term = moved[HALO : HALO + length] * table[k : k + 1].astype(F32)
        total = term if total is None else total + term
    return total


def silu(v):
    return v * jax.nn.sigmoid(v)


def mix_kernel(
    og_ref, ig_ref, va_ref, x_ref, b_ref, c_ref, ct_ref, xt_ref, bt_ref, rt_ref,
    col_ref, row_ref, yconv_ref, within_ref, reads_ref, state_ref,
):
    length = yconv_ref.shape[0]
    gated = (ig_ref[...].astype(F32) * va_ref[...].astype(F32)).astype(BF16).astype(F32)
    conv = taps_of(gated, ct_ref[...], length)
    yconv_ref[...] = (og_ref[pl.ds(HALO, length), :].astype(F32) * conv).astype(BF16)
    xs = silu(taps_of(x_ref[...].astype(F32), xt_ref[...], length)).astype(BF16)
    bs = silu(taps_of(b_ref[...].astype(F32), bt_ref[...], length)).astype(BF16)
    cs = silu(taps_of(c_ref[...].astype(F32), rt_ref[...], length)).astype(BF16)
    reads_ref[...] = cs
    cols = col_ref[0]
    rows = row_ref[0]
    t_at = lax.broadcasted_iota(jnp.int32, (length, length), 0)
    s_at = lax.broadcasted_iota(jnp.int32, (length, length), 1)
    outs, weighted = [], []
    for h in range(2):
        c_h = cs[:, h * STATE : (h + 1) * STATE]
        b_h = bs[:, h * STATE : (h + 1) * STATE]
        x_h = xs[:, h * HEAD_DIM : (h + 1) * HEAD_DIM]
        o = 4 * h
        scores = lax.dot_general(
            c_h, b_h, (((1,), (1,)), ((), ())), preferred_element_type=F32
        )
        gap = jnp.where(
            t_at >= s_at,
            cols[:, o + 2 : o + 3] - rows[o + 2 : o + 3],
            cols[:, o + 3 : o + 4] - rows[o + 3 : o + 4],
        )
        d_f, d_b = rows[o : o + 1], rows[o + 1 : o + 2]
        scale = jnp.where(t_at > s_at, d_f, jnp.where(t_at < s_at, d_b, d_f + d_b))
        w = (scores * jnp.exp(gap) * scale).astype(BF16)
        outs.append(jnp.dot(w, x_h, preferred_element_type=F32))
        x32 = x_h.astype(F32)
        end_f = jnp.exp(rows[o + 2 : o + 3, length - 1 : length] - cols[:, o + 2 : o + 3])
        end_b = jnp.exp(rows[o + 3 : o + 4, 0:1] - cols[:, o + 3 : o + 4])
        both = jnp.concatenate(
            [x32 * (end_f * cols[:, o : o + 1]), x32 * (end_b * cols[:, o + 1 : o + 2])], axis=1
        ).astype(BF16)
        state_ref[h * STATE : (h + 1) * STATE] = lax.dot_general(
            both, b_h, (((0,), (0,)), ((), ())), preferred_element_type=F32
        ).astype(BF16)
    within_ref[...] = jnp.concatenate(outs, axis=1)


def chain_kernel(s_ref, d_ref, back_ref, out_ref):
    n = s_ref.shape[0]
    back = back_ref[...] > 0.5
    acc = jnp.zeros(s_ref.shape[1:], F32)
    fwd = []
    for j in range(n):
        fwd.append(acc)
        acc = acc * d_ref[j] + s_ref[j].astype(F32)
    acc = jnp.zeros(s_ref.shape[1:], F32)
    for j in reversed(range(n)):
        out_ref[j] = jnp.where(back, acc, fwd[j]).astype(BF16)
        acc = acc * d_ref[j] + s_ref[j].astype(F32)


def finish_kernel(within_ref, reads_ref, enter_ref, gate_ref, gain_ref, col_ref, y_ref):
    length = y_ref.shape[0]
    cols = col_ref[0]
    outs = []
    for h in range(2):
        o = 4 * h
        both = lax.dot_general(
            reads_ref[:, h * STATE : (h + 1) * STATE],
            enter_ref[h * STATE : (h + 1) * STATE],
            (((1,), (1,)), ((), ())),
            preferred_element_type=F32,
        )
        here = slice(h * HEAD_DIM, (h + 1) * HEAD_DIM)
        y = within_ref[:, here]
        y = y + both[:, :HEAD_DIM] * jnp.exp(cols[:, o + 2 : o + 3])
        y = y + both[:, HEAD_DIM:] * jnp.exp(cols[:, o + 3 : o + 4])
        g = y * silu(gate_ref[pl.ds(HALO, length), :].astype(F32)[:, here])
        g = g * lax.rsqrt(jnp.mean(g * g, axis=-1, keepdims=True) + epsilon)
        outs.append(g * gain_ref[:, here].astype(F32))
    y_ref[...] = jnp.concatenate(outs, axis=1).astype(BF16)


def local(
    layer_source_rows, entry_rescale_factor, sliding_mixer_entry_matrix,
    recurrent_mixer_entry_matrix, latent_write_read_matrix, timestep_matrix,
    sliding_kernel_coefficients, recurrent_kernel_coefficients, latent_kernel_coefficients,
    lane_forgetting_rate, spike_forgetting_rate, lane_rescale_factor,
    sliding_mixer_exit_matrix, recurrent_mixer_exit_matrix,
):
    n = lax.axis_size("sp")
    tp = lax.axis_size("tp")
    own_rows, width = layer_source_rows.shape
    length = own_rows * tp
    full = length + 2 * HALO
    conv_width = sliding_mixer_entry_matrix.shape[2]
    ssd_width = recurrent_mixer_entry_matrix.shape[2]
    state_width = latent_write_read_matrix.shape[2]
    heads = timestep_matrix.shape[2]
    pairs = heads // 2
    cw = conv_width // pairs

    block = jnp.concatenate(
        [sliding_mixer_entry_matrix[i] for i in range(3)]
        + [recurrent_mixer_entry_matrix[i] for i in range(2)]
        + [latent_write_read_matrix[i] for i in range(2)],
        axis=1,
    )
    gathered = gather_rows(block)
    weights = gathered.reshape(n * block.shape[0], block.shape[1])

    x32 = layer_source_rows.astype(F32)
    normed = (
        x32
        * lax.rsqrt(jnp.mean(x32 * x32, axis=-1, keepdims=True) + epsilon)
        * entry_rescale_factor.astype(F32)
    ).astype(BF16)
    up = [(i, i + 1) for i in range(n - 1)]
    down = [(i + 1, i) for i in range(n - 1)]
    before = lax.ppermute(normed[own_rows - HALO :], "sp", up)
    after = lax.ppermute(normed[:HALO], "sp", down)
    shared = lax.all_gather(jnp.concatenate([before, normed, after], axis=0), "tp", axis=0)
    rows = jnp.concatenate(
        [shared[tp - 1, :HALO]]
        + [shared[i, HALO : HALO + own_rows] for i in range(tp)]
        + [shared[0, HALO + own_rows :]],
        axis=0,
    )

    step_weight = timestep_matrix.reshape(width, 2 * heads)
    raw = jnp.dot(rows, step_weight, preferred_element_type=F32).astype(BF16)
    raw = raw[HALO : HALO + length].astype(F32).reshape(length, 2, heads)
    deltas = jax.nn.softplus(raw)
    logs = -deltas * lane_forgetting_rate[None] + spike_forgetting_rate[:, None, :]
    tri = (jnp.arange(length)[:, None] >= jnp.arange(length)[None, :]).astype(F32)
    run_f = jnp.dot(tri, logs[:, 0], precision=HIGHEST)
    run_b = jnp.dot(tri.T, logs[:, 1], precision=HIGHEST)
    table = jnp.stack([deltas[:, 0], deltas[:, 1], run_f, run_b], axis=2)
    col_table = table.reshape(length, pairs, 8).transpose(1, 0, 2)
    row_table = table.reshape(length, pairs, 8).transpose(1, 2, 0)
    span_log = jnp.stack([run_f[length - 1], run_b[0]], axis=1)
    span_decay = jnp.exp(lax.all_gather(span_log, "sp")).reshape(n, heads * 2)
    span_decay = jnp.repeat(span_decay, HEAD_DIM, axis=1)
    share = heads * 2 * HEAD_DIM // n
    mine = lax.axis_index("sp") * share
    chain_decay = lax.dynamic_slice_in_dim(span_decay, mine, share, axis=1)[:, :, None]
    chain_back = ((mine + jnp.arange(share)) // HEAD_DIM % 2).astype(F32)[:, None]

    rows, weights = lax.optimization_barrier((rows, weights))
    proj = jnp.dot(rows, weights, preferred_element_type=F32).astype(BF16)

    exit_c, exit_s, proj = lax.optimization_barrier(
        (sliding_mixer_exit_matrix, recurrent_mixer_exit_matrix, proj)
    )
    exit_c = lax.all_gather(exit_c, "sp", axis=1, tiled=True)
    exit_s = lax.all_gather(exit_s, "sp", axis=1, tiled=True)

    latent = latent_kernel_coefficients
    pw, sw = 2 * HEAD_DIM, 2 * STATE
    g0 = 3 * conv_width
    at_gate, at_x = g0 // pw, (g0 + ssd_width) // pw
    at_b = (g0 + 2 * ssd_width) // sw
    at_c = at_b + pairs
    y_conv, within, reads, states = pl.pallas_call(
        mix_kernel,
        grid=(pairs,),
        in_specs=[
            pl.BlockSpec((full, cw), lambda j: (0, j)),
            pl.BlockSpec((full, cw), lambda j: (0, pairs + j)),
            pl.BlockSpec((full, cw), lambda j: (0, 2 * pairs + j)),
            pl.BlockSpec((full, pw), lambda j: (0, at_x + j)),
            pl.BlockSpec((full, sw), lambda j: (0, at_b + j)),
            pl.BlockSpec((full, sw), lambda j: (0, at_c + j)),
            pl.BlockSpec((3, cw), lambda j: (0, j)),
            pl.BlockSpec((5, pw), lambda j: (0, j)),
            pl.BlockSpec((5, sw), lambda j: (0, j)),
            pl.BlockSpec((5, sw), lambda j: (0, pairs + j)),
            pl.BlockSpec((1, length, 8), lambda j: (j, 0, 0)),
            pl.BlockSpec((1, 8, length), lambda j: (j, 0, 0)),
        ],
        out_specs=[
            pl.BlockSpec((length, cw), lambda j: (0, j)),
            pl.BlockSpec((length, pw), lambda j: (0, j)),
            pl.BlockSpec((length, sw), lambda j: (0, j)),
            pl.BlockSpec((sw, STATE), lambda j: (j, 0)),
        ],
        out_shape=[
            jax.ShapeDtypeStruct((length, conv_width), BF16),
            jax.ShapeDtypeStruct((length, ssd_width), F32),
            jax.ShapeDtypeStruct((length, state_width), BF16),
            jax.ShapeDtypeStruct((pairs * sw, STATE), BF16),
        ],
        cost_estimate=pl.CostEstimate(
            flops=8 * length * length * heads * STATE, bytes_accessed=2**24, transcendentals=0
        ),
    )(
        proj, proj, proj, proj, proj, proj,
        sliding_kernel_coefficients, recurrent_kernel_coefficients,
        latent.reshape(latent.shape[0], -1), latent.reshape(latent.shape[0], -1),
        col_table, row_table,
    )

    pieces = lax.all_to_all(states.reshape(n, share, STATE), "sp", 0, 0)
    entering = pl.pallas_call(
        chain_kernel, out_shape=jax.ShapeDtypeStruct((n, share, STATE), BF16)
    )(pieces, chain_decay, chain_back)
    entering = lax.all_to_all(entering, "sp", 0, 0).reshape(pairs * sw, STATE)

    y_ssd = pl.pallas_call(
        finish_kernel,
        grid=(pairs,),
        in_specs=[
            pl.BlockSpec((length, pw), lambda j: (0, j)),
            pl.BlockSpec((length, sw), lambda j: (0, j)),
            pl.BlockSpec((sw, STATE), lambda j: (j, 0)),
            pl.BlockSpec((full, pw), lambda j: (0, at_gate + j)),
            pl.BlockSpec((1, pw), lambda j: (0, j)),
            pl.BlockSpec((1, length, 8), lambda j: (j, 0, 0)),
        ],
        out_specs=pl.BlockSpec((length, pw), lambda j: (0, j)),
        out_shape=jax.ShapeDtypeStruct((length, ssd_width), BF16),
    )(within, reads, entering, proj, lane_rescale_factor.reshape(1, -1), col_table)

    partial = (
        jnp.dot(y_conv, exit_c, preferred_element_type=F32)
        + jnp.dot(y_ssd, exit_s, preferred_element_type=F32)
    ).astype(BF16)
    return lax.psum_scatter(partial, "tp", scatter_dimension=0, tiled=True)


def solution(mesh):
    placed = (
        P(("sp", "tp"), None),
        P(),
        P(None, "sp", "tp"),
        P(None, "sp", "tp"),
        P(None, "sp", "tp"),
        P(None, None, "tp"),
        P(None, "tp"),
        P(None, "tp"),
        P(None, None, "tp"),
        P(None, "tp"),
        P("sp", "tp"),
        P("tp"),
        P("tp", "sp"),
        P("tp", "sp"),
    )
    return jax.shard_map(
        local, mesh=mesh, in_specs=placed, out_specs=P(("sp", "tp"), None), check_vma=False
    )
```

```python
import functools

import jax
import jax.numpy as jnp
from jax import lax
from jax.experimental import pallas as pl
from jax.experimental.pallas import tpu as pltpu
from jax.sharding import PartitionSpec as P

HEAD_DIM = 64
STATE = 128
HALO = 8
CHUNKS = 2
epsilon = 1e-05
F32 = jnp.float32
BF16 = jnp.bfloat16
HIGHEST = lax.Precision.HIGHEST


def ring_kernel(n, w_ref, out_ref, own_sem, ring_send, ring_recv, mate_send, mate_recv):
    chips = n // 2
    me = lax.axis_index("sp")
    core, chip = me % 2, me // 2
    odd = chip % 2
    spot = (1 - odd) * (chip // 2) + odd * (chips - 1 - chip // 2)

    def device(position):
        position = (position + 2 * chips) % chips
        half = (chips + 1) // 2
        late = position // half
        late_chip = 2 * (chips - 1 - position) + 1
        return 2 * ((1 - late) * 2 * position + late * late_chip) + core

    mate = me + 1 - 2 * core
    ways = (device(spot + 1), device(spot - 1))
    rows = w_ref.shape[0] // (2 * CHUNKS)

    barrier = pltpu.get_barrier_semaphore()
    for other in (mate,) + ways:
        pl.semaphore_signal(
            barrier, inc=1, device_id={"sp": other}, device_id_type=pl.DeviceIdType.MESH
        )
    pl.semaphore_wait(barrier, 3)

    def piece(way, chunk):
        return pl.ds((way * CHUNKS + chunk) * rows, rows)

    def ring_copy(step, way, chunk):
        owner = device(spot - step if way == 0 else spot + step)
        part = piece(way, chunk)
        return pltpu.make_async_remote_copy(
            src_ref=w_ref.at[part] if step == 0 else out_ref.at[owner, part],
            dst_ref=out_ref.at[owner, part],
            send_sem=ring_send.at[step, way, chunk],
            recv_sem=ring_recv.at[step, way, chunk],
            device_id={"sp": ways[way]},
            device_id_type=pl.DeviceIdType.MESH,
        )

    def arrival(step, way, chunk):
        owner = device(spot - step - 1 if way == 0 else spot + step + 1)
        part = piece(way, chunk)
        return pltpu.make_async_remote_copy(
            src_ref=out_ref.at[owner, part],
            dst_ref=out_ref.at[owner, part],
            send_sem=ring_send.at[step, way, chunk],
            recv_sem=ring_recv.at[step, way, chunk],
            device_id={"sp": ways[way]},
            device_id_type=pl.DeviceIdType.MESH,
        )

    def mate_copy(step, way, chunk, incoming=False):
        owner = device(spot - step if way == 0 else spot + step)
        if incoming:
            owner = owner + 1 - 2 * core
        part = piece(way, chunk)
        return pltpu.make_async_remote_copy(
            src_ref=w_ref.at[part] if step == 0 else out_ref.at[owner, part],
            dst_ref=out_ref.at[owner, part],
            send_sem=mate_send.at[step, way, chunk],
            recv_sem=mate_recv.at[step, way, chunk],
            device_id={"sp": mate},
            device_id_type=pl.DeviceIdType.MESH,
        )

    parts = [(way, chunk) for chunk in range(CHUNKS) for way in range(2)]
    for way, chunk in parts:
        ring_copy(0, way, chunk).start()
    for way, chunk in parts:
        mate_copy(0, way, chunk).start()
    own = pltpu.make_async_copy(w_ref, out_ref.at[me], own_sem)
    own.start()
    for step in range(chips - 1):
        for way, chunk in parts:
            arrival(step, way, chunk).wait_recv()
            if step < chips - 2:
                ring_copy(step + 1, way, chunk).start()
            mate_copy(step + 1, way, chunk).start()
    own.wait()
    for step in range(chips):
        for way, chunk in parts:
            if step < chips - 1:
                ring_copy(step, way, chunk).wait_send()
            mate_copy(step, way, chunk).wait_send()
            mate_copy(step, way, chunk, True).wait_recv()


def gather_rows(block):
    n = lax.axis_size("sp")
    chips = n // 2
    rows, cols = block.shape
    return pl.pallas_call(
        functools.partial(ring_kernel, n),
        out_shape=jax.ShapeDtypeStruct((n, rows, cols), block.dtype),
        in_specs=[pl.BlockSpec(memory_space=pltpu.VMEM)],
        out_specs=pl.BlockSpec(memory_space=pl.ANY),
        scratch_shapes=[
            pltpu.SemaphoreType.DMA,
            pltpu.SemaphoreType.DMA((chips - 1, 2, CHUNKS)),
            pltpu.SemaphoreType.DMA((chips - 1, 2, CHUNKS)),
            pltpu.SemaphoreType.DMA((chips, 2, CHUNKS)),
            pltpu.SemaphoreType.DMA((chips, 2, CHUNKS)),
        ],
        compiler_params=pltpu.CompilerParams(
            collective_id=0, has_side_effects=True, vmem_limit_bytes=16 * 2**20
        ),
        cost_estimate=pl.CostEstimate(
            flops=0, bytes_accessed=n * rows * cols * 16, transcendentals=0
        ),
    )(block)


def taps_of(padded, table, length):
    full = padded.shape[0]
    half = table.shape[0] // 2
    total = None
    for k in range(table.shape[0]):
        moved = padded if k == half else pltpu.roll(padded, (half - k) % full, 0)
        term = moved[HALO : HALO + length] * table[k : k + 1].astype(F32)
        total = term if total is None else total + term
    return total


def silu(v):
    return v * jax.nn.sigmoid(v)


def mix_kernel(
    og_ref, ig_ref, va_ref, x_ref, b_ref, c_ref, ct_ref, xt_ref, bt_ref, rt_ref,
    col_ref, row_ref, yconv_ref, within_ref, reads_ref, state_ref,
):
    length = yconv_ref.shape[0]
    gated = (ig_ref[...].astype(F32) * va_ref[...].astype(F32)).astype(BF16).astype(F32)
    conv = taps_of(gated, ct_ref[...], length)
    yconv_ref[...] = (og_ref[pl.ds(HALO, length), :].astype(F32) * conv).astype(BF16)
    xs = silu(taps_of(x_ref[...].astype(F32), xt_ref[...], length)).astype(BF16)
    bs = silu(taps_of(b_ref[...].astype(F32), bt_ref[...], length)).astype(BF16)
    cs = silu(taps_of(c_ref[...].astype(F32), rt_ref[...], length)).astype(BF16)
    reads_ref[...] = cs
    cols = col_ref[0]
    rows = row_ref[0]
    t_at = lax.broadcasted_iota(jnp.int32, (length, length), 0)
    s_at = lax.broadcasted_iota(jnp.int32, (length, length), 1)
    outs, weighted = [], []
    for h in range(2):
        c_h = cs[:, h * STATE : (h + 1) * STATE]
        b_h = bs[:, h * STATE : (h + 1) * STATE]
        x_h = xs[:, h * HEAD_DIM : (h + 1) * HEAD_DIM]
        o = 4 * h
        scores = lax.dot_general(
            c_h, b_h, (((1,), (1,)), ((), ())), preferred_element_type=F32
        )
        gap = jnp.where(
            t_at >= s_at,
            cols[:, o + 2 : o + 3] - rows[o + 2 : o + 3],
            cols[:, o + 3 : o + 4] - rows[o + 3 : o + 4],
        )
        d_f, d_b = rows[o : o + 1], rows[o + 1 : o + 2]
        scale = jnp.where(t_at > s_at, d_f, jnp.where(t_at < s_at, d_b, d_f + d_b))
        w = (scores * jnp.exp(gap) * scale).astype(BF16)
        outs.append(jnp.dot(w, x_h, preferred_element_type=F32))
        x32 = x_h.astype(F32)
        end_f = jnp.exp(rows[o + 2 : o + 3, length - 1 : length] - cols[:, o + 2 : o + 3])
        end_b = jnp.exp(rows[o + 3 : o + 4, 0:1] - cols[:, o + 3 : o + 4])
        both = jnp.concatenate(
            [x32 * (end_f * cols[:, o : o + 1]), x32 * (end_b * cols[:, o + 1 : o + 2])], axis=1
        ).astype(BF16)
        state_ref[h * STATE : (h + 1) * STATE] = lax.dot_general(
            both, b_h, (((0,), (0,)), ((), ())), preferred_element_type=F32
        ).astype(BF16)
    within_ref[...] = jnp.concatenate(outs, axis=1)


def exchange_kernel(
    n, share, s_ref, l_ref, out_ref, got, logs, enter, s_out, s_in, l_out, l_in, e_out, e_in
):
    me = lax.axis_index("sp")
    barrier = pltpu.get_barrier_semaphore()
    for k in range(1, n):
        pl.semaphore_signal(
            barrier,
            inc=1,
            device_id={"sp": (me + k) % n},
            device_id_type=pl.DeviceIdType.MESH,
        )
    pl.semaphore_wait(barrier, n - 1)

    def copy(src, dst, out_sem, in_sem, k, there, slot):
        return pltpu.make_async_remote_copy(
            src_ref=src.at[there],
            dst_ref=dst.at[slot],
            send_sem=out_sem.at[k],
            recv_sem=in_sem.at[k],
            device_id={"sp": there},
            device_id_type=pl.DeviceIdType.MESH,
        )

    for k in range(1, n):
        there = (me + k) % n
        copy(s_ref, got, s_out, s_in, k, there, me).start()
        copy(l_ref, logs, l_out, l_in, k, there, me).start()
    got[me] = s_ref[me]
    logs[me] = l_ref[me]
    for k in range(1, n):
        here = (me + n - k) % n
        copy(s_ref, got, s_out, s_in, k, here, here).wait_recv()
        copy(l_ref, logs, l_out, l_in, k, here, here).wait_recv()
    back = (me * share // HEAD_DIM) % 2
    acc = jnp.zeros(s_ref.shape[1:], F32)
    for i in range(n):
        j = back * (n - 1 - i) + (1 - back) * i
        enter[j] = acc.astype(BF16)
        acc = acc * jnp.exp(logs[j][0:1, :]) + got[j].astype(F32)
    out_ref[me] = enter[me]
    for k in range(1, n):
        copy(enter, out_ref, e_out, e_in, k, (me + k) % n, me).start()
    for k in range(1, n):
        here = (me + n - k) % n
        copy(enter, out_ref, e_out, e_in, k, here, here).wait_recv()
    for k in range(1, n):
        there = (me + k) % n
        copy(s_ref, got, s_out, s_in, k, there, me).wait_send()
        copy(l_ref, logs, l_out, l_in, k, there, me).wait_send()
        copy(enter, out_ref, e_out, e_in, k, there, me).wait_send()


def exchange_states(states, span_log):
    n, share, _ = states.shape
    assert HEAD_DIM % share == 0
    tables = jnp.repeat(span_log.reshape(-1), HEAD_DIM // share)
    tables = jnp.broadcast_to(tables[:, None, None], (n, 8, STATE))
    return pl.pallas_call(
        functools.partial(exchange_kernel, n, share),
        out_shape=jax.ShapeDtypeStruct(states.shape, BF16),
        in_specs=[pl.BlockSpec(memory_space=pltpu.VMEM)] * 2,
        out_specs=pl.BlockSpec(memory_space=pltpu.VMEM),
        scratch_shapes=[
            pltpu.VMEM(states.shape, BF16),
            pltpu.VMEM(tables.shape, F32),
            pltpu.VMEM(states.shape, BF16),
        ]
        + [pltpu.SemaphoreType.DMA((n,))] * 6,
        compiler_params=pltpu.CompilerParams(collective_id=1, has_side_effects=True),
        cost_estimate=pl.CostEstimate(flops=0, bytes_accessed=2**25, transcendentals=0),
    )(states, tables)


def project_kernel(r_ref, w_ref, o_ref):
    o_ref[...] = jnp.dot(r_ref[...], w_ref[...], preferred_element_type=F32).astype(BF16)


def project(rows, weights):
    count, width = rows.shape
    cols = weights.shape[1]
    tile = cols // 9
    return pl.pallas_call(
        project_kernel,
        grid=(9,),
        in_specs=[
            pl.BlockSpec((count, width), lambda j: (0, 0)),
            pl.BlockSpec((width, tile), lambda j: (0, j)),
        ],
        out_specs=pl.BlockSpec((count, tile), lambda j: (0, j)),
        out_shape=jax.ShapeDtypeStruct((count, cols), BF16),
        cost_estimate=pl.CostEstimate(
            flops=2 * count * width * cols, bytes_accessed=2 * width * cols, transcendentals=0
        ),
    )(rows, weights)


def finish_kernel(within_ref, reads_ref, enter_ref, gate_ref, gain_ref, col_ref, y_ref):
    length = y_ref.shape[0]
    cols = col_ref[0]
    outs = []
    for h in range(2):
        o = 4 * h
        both = lax.dot_general(
            reads_ref[:, h * STATE : (h + 1) * STATE],
            enter_ref[h * STATE : (h + 1) * STATE],
            (((1,), (1,)), ((), ())),
            preferred_element_type=F32,
        )
        here = slice(h * HEAD_DIM, (h + 1) * HEAD_DIM)
        y = within_ref[:, here]
        y = y + both[:, :HEAD_DIM] * jnp.exp(cols[:, o + 2 : o + 3])
        y = y + both[:, HEAD_DIM:] * jnp.exp(cols[:, o + 3 : o + 4])
        g = y * silu(gate_ref[pl.ds(HALO, length), :].astype(F32)[:, here])
        g = g * lax.rsqrt(jnp.mean(g * g, axis=-1, keepdims=True) + epsilon)
        outs.append(g * gain_ref[:, here].astype(F32))
    y_ref[...] = jnp.concatenate(outs, axis=1).astype(BF16)


def local(
    layer_source_rows, entry_rescale_factor, sliding_mixer_entry_matrix,
    recurrent_mixer_entry_matrix, latent_write_read_matrix, timestep_matrix,
    sliding_kernel_coefficients, recurrent_kernel_coefficients, latent_kernel_coefficients,
    lane_forgetting_rate, spike_forgetting_rate, lane_rescale_factor,
    sliding_mixer_exit_matrix, recurrent_mixer_exit_matrix,
):
    n = lax.axis_size("sp")
    tp = lax.axis_size("tp")
    own_rows, width = layer_source_rows.shape
    length = own_rows * tp
    full = length + 2 * HALO
    conv_width = sliding_mixer_entry_matrix.shape[2]
    ssd_width = recurrent_mixer_entry_matrix.shape[2]
    state_width = latent_write_read_matrix.shape[2]
    heads = timestep_matrix.shape[2]
    pairs = heads // 2
    cw = conv_width // pairs

    block = jnp.concatenate(
        [sliding_mixer_entry_matrix[i] for i in range(3)]
        + [recurrent_mixer_entry_matrix[i] for i in range(2)]
        + [latent_write_read_matrix[i] for i in range(2)],
        axis=1,
    )
    gathered = gather_rows(block)
    weights = gathered.reshape(n * block.shape[0], block.shape[1])

    x32 = layer_source_rows.astype(F32)
    normed = (
        x32
        * lax.rsqrt(jnp.mean(x32 * x32, axis=-1, keepdims=True) + epsilon)
        * entry_rescale_factor.astype(F32)
    ).astype(BF16)
    up = [(i, i + 1) for i in range(n - 1)]
    down = [(i + 1, i) for i in range(n - 1)]
    before = lax.ppermute(normed[own_rows - HALO :], "sp", up)
    after = lax.ppermute(normed[:HALO], "sp", down)
    shared = lax.all_gather(jnp.concatenate([before, normed, after], axis=0), "tp", axis=0)
    rows = jnp.concatenate(
        [shared[tp - 1, :HALO]]
        + [shared[i, HALO : HALO + own_rows] for i in range(tp)]
        + [shared[0, HALO + own_rows :]],
        axis=0,
    )

    step_weight = timestep_matrix.reshape(width, 2 * heads)
    raw = jnp.dot(rows, step_weight, preferred_element_type=F32).astype(BF16)
    raw = raw[HALO : HALO + length].astype(F32).reshape(length, 2, heads)
    deltas = jax.nn.softplus(raw)
    logs = -deltas * lane_forgetting_rate[None] + spike_forgetting_rate[:, None, :]
    tri = (jnp.arange(length)[:, None] >= jnp.arange(length)[None, :]).astype(F32)
    run_f = jnp.dot(tri, logs[:, 0], precision=HIGHEST)
    run_b = jnp.dot(tri.T, logs[:, 1], precision=HIGHEST)
    table = jnp.stack([deltas[:, 0], deltas[:, 1], run_f, run_b], axis=2)
    col_table = table.reshape(length, pairs, 8).transpose(1, 0, 2)
    row_table = table.reshape(length, pairs, 8).transpose(1, 2, 0)
    span_log = jnp.stack([run_f[length - 1], run_b[0]], axis=1)
    share = heads * 2 * HEAD_DIM // n

    exit_c, exit_s, weights = lax.optimization_barrier(
        (sliding_mixer_exit_matrix, recurrent_mixer_exit_matrix, weights)
    )
    proj = project(rows, weights)
    exit_c = lax.all_gather(exit_c, "sp", axis=1, tiled=True)
    exit_s = lax.all_gather(exit_s, "sp", axis=1, tiled=True)

    latent = latent_kernel_coefficients
    pw, sw = 2 * HEAD_DIM, 2 * STATE
    g0 = 3 * conv_width
    at_gate, at_x = g0 // pw, (g0 + ssd_width) // pw
    at_b = (g0 + 2 * ssd_width) // sw
    at_c = at_b + pairs
    y_conv, within, reads, states = pl.pallas_call(
        mix_kernel,
        grid=(pairs,),
        in_specs=[
            pl.BlockSpec((full, cw), lambda j: (0, j)),
            pl.BlockSpec((full, cw), lambda j: (0, pairs + j)),
            pl.BlockSpec((full, cw), lambda j: (0, 2 * pairs + j)),
            pl.BlockSpec((full, pw), lambda j: (0, at_x + j)),
            pl.BlockSpec((full, sw), lambda j: (0, at_b + j)),
            pl.BlockSpec((full, sw), lambda j: (0, at_c + j)),
            pl.BlockSpec((3, cw), lambda j: (0, j)),
            pl.BlockSpec((5, pw), lambda j: (0, j)),
            pl.BlockSpec((5, sw), lambda j: (0, j)),
            pl.BlockSpec((5, sw), lambda j: (0, pairs + j)),
            pl.BlockSpec((1, length, 8), lambda j: (j, 0, 0)),
            pl.BlockSpec((1, 8, length), lambda j: (j, 0, 0)),
        ],
        out_specs=[
            pl.BlockSpec((length, cw), lambda j: (0, j)),
            pl.BlockSpec((length, pw), lambda j: (0, j)),
            pl.BlockSpec((length, sw), lambda j: (0, j)),
            pl.BlockSpec((sw, STATE), lambda j: (j, 0)),
        ],
        out_shape=[
            jax.ShapeDtypeStruct((length, conv_width), BF16),
            jax.ShapeDtypeStruct((length, ssd_width), F32),
            jax.ShapeDtypeStruct((length, state_width), BF16),
            jax.ShapeDtypeStruct((pairs * sw, STATE), BF16),
        ],
        cost_estimate=pl.CostEstimate(
            flops=8 * length * length * heads * STATE, bytes_accessed=2**24, transcendentals=0
        ),
    )(
        proj, proj, proj, proj, proj, proj,
        sliding_kernel_coefficients, recurrent_kernel_coefficients,
        latent.reshape(latent.shape[0], -1), latent.reshape(latent.shape[0], -1),
        col_table, row_table,
    )

    entering = exchange_states(states.reshape(n, share, STATE), span_log)
    entering = entering.reshape(pairs * sw, STATE)

    y_ssd = pl.pallas_call(
        finish_kernel,
        grid=(pairs,),
        in_specs=[
            pl.BlockSpec((length, pw), lambda j: (0, j)),
            pl.BlockSpec((length, sw), lambda j: (0, j)),
            pl.BlockSpec((sw, STATE), lambda j: (j, 0)),
            pl.BlockSpec((full, pw), lambda j: (0, at_gate + j)),
            pl.BlockSpec((1, pw), lambda j: (0, j)),
            pl.BlockSpec((1, length, 8), lambda j: (j, 0, 0)),
        ],
        out_specs=pl.BlockSpec((length, pw), lambda j: (0, j)),
        out_shape=jax.ShapeDtypeStruct((length, ssd_width), BF16),
    )(within, reads, entering, proj, lane_rescale_factor.reshape(1, -1), col_table)

    def partial(y_c, y_s):
        return (
            jnp.dot(y_c, exit_c, preferred_element_type=F32)
            + jnp.dot(y_s, exit_s, preferred_element_type=F32)
        ).astype(BF16)

    if tp != 2:
        return lax.psum_scatter(
            partial(y_conv, y_ssd), "tp", scatter_dimension=0, tiled=True
        )
    tp_me = lax.axis_index("tp")

    def rows_of(owner, y):
        return lax.dynamic_slice_in_dim(y, owner * own_rows, own_rows, axis=0)

    away = partial(rows_of(1 - tp_me, y_conv), rows_of(1 - tp_me, y_ssd))
    arrived = lax.ppermute(away, "tp", [(0, 1), (1, 0)])
    kept = partial(rows_of(tp_me, y_conv), rows_of(tp_me, y_ssd))
    return (kept.astype(F32) + arrived.astype(F32)).astype(BF16)


def solution(mesh):
    placed = (
        P(("sp", "tp"), None),
        P(),
        P(None, "sp", "tp"),
        P(None, "sp", "tp"),
        P(None, "sp", "tp"),
        P(None, None, "tp"),
        P(None, "tp"),
        P(None, "tp"),
        P(None, None, "tp"),
        P(None, "tp"),
        P("sp", "tp"),
        P("tp"),
        P("tp", "sp"),
        P("tp", "sp"),
    )
    return jax.shard_map(
        local, mesh=mesh, in_specs=placed, out_specs=P(("sp", "tp"), None), check_vma=False
    )
```

```python
import functools

import jax
import jax.numpy as jnp
from jax import lax
from jax.experimental import pallas as pl
from jax.experimental.pallas import tpu as pltpu
from jax.sharding import PartitionSpec as P

HEAD_DIM = 64
STATE = 128
HALO = 16
CHUNKS = 2
epsilon = 1e-05
F32 = jnp.float32
BF16 = jnp.bfloat16
HIGHEST = lax.Precision.HIGHEST


def entry_kernel(
    n, tp, w_ref, x_ref, proj_ref, rows_ref, wbuf, rows, acc, own_sem, ring_send, ring_recv,
    mate_send, mate_recv, row_sem, row_recv, edge_send, edge_recv,
):
    chips = n // 2
    me = lax.axis_index("sp")
    core, chip = me % 2, me // 2
    odd = chip % 2
    spot = (1 - odd) * (chip // 2) + odd * (chips - 1 - chip // 2)
    depth, cols = w_ref.shape
    full = proj_ref.shape[0]
    own_rows = x_ref.shape[0]

    def chip_at(position):
        position = (position + 2 * chips) % chips
        late = position // ((chips + 1) // 2)
        return (1 - late) * 2 * position + late * (2 * (chips - 1 - position) + 1)

    def device(position):
        return 2 * chip_at(position) + core

    mate = me + 1 - 2 * core
    ways = (device(spot + 1), device(spot - 1))
    cut = (cols // 128 + 1) // 2 * 128
    spans = ((0, cut), (cut, cols - cut))
    part_rows = depth // CHUNKS
    mesh_id = pl.DeviceIdType.MESH

    barrier = pltpu.get_barrier_semaphore()
    for other in (mate,) + ways:
        pl.semaphore_signal(barrier, inc=1, device_id={"sp": other}, device_id_type=mesh_id)
    greeted = 3
    if tp == 2:
        side = lax.axis_index("tp")
        for there in (
            {"tp": 1 - side},
            {"sp": (me + n - 1) % n, "tp": 1},
            {"sp": (me + 1) % n, "tp": 0},
        ):
            pl.semaphore_signal(barrier, inc=1, device_id=there, device_id_type=mesh_id)
        greeted = 6
    pl.semaphore_wait(barrier, greeted)

    def view(ref, owner, way, chunk):
        start, size = spans[way]
        part = pl.ds(chunk * part_rows, part_rows)
        if owner is None:
            return ref.at[part, pl.ds(start, size)]
        return ref.at[owner, part, pl.ds(start, size)]

    def owner_of(step, way):
        return device(spot - step if way == 0 else spot + step)

    def send(step, way, chunk, owner, out_sem, in_sem, there):
        return pltpu.make_async_remote_copy(
            src_ref=view(w_ref, None, way, chunk) if step == 0 else view(wbuf, owner, way, chunk),
            dst_ref=view(wbuf, owner, way, chunk),
            send_sem=out_sem,
            recv_sem=in_sem,
            device_id={"sp": there},
            device_id_type=mesh_id,
        )

    def ring_copy(step, way, chunk):
        at = (step, way, chunk)
        owner = owner_of(step, way)
        return send(*at, owner, ring_send.at[at], ring_recv.at[at], ways[way])

    def arrival(step, way, chunk):
        at = (step, way, chunk)
        owner = owner_of(step + 1, way)
        return send(1, way, chunk, owner, ring_send.at[at], ring_recv.at[at], ways[way])

    def mate_copy(step, way, chunk, incoming=False):
        at = (step, way, chunk)
        owner = owner_of(step, way)
        if incoming:
            owner = owner + 1 - 2 * core
        return send(*at, owner, mate_send.at[at], mate_recv.at[at], mate)

    parts = [(way, chunk) for chunk in range(CHUNKS) for way in range(2)]
    for way, chunk in parts:
        ring_copy(0, way, chunk).start()
    for way, chunk in parts:
        mate_copy(0, way, chunk).start()
    own = pltpu.make_async_copy(w_ref, wbuf.at[me], own_sem.at[0])
    own.start()

    if tp == 2:
        place = pl.ds(HALO + pl.multiple_of(side * own_rows, HALO), own_rows)
        other_place = pl.ds(HALO + pl.multiple_of((1 - side) * own_rows, HALO), own_rows)
        mine = pltpu.make_async_copy(x_ref, rows.at[place], own_sem.at[1])
        mine.start()

        def row_copy(where):
            return pltpu.make_async_remote_copy(
                src_ref=x_ref,
                dst_ref=rows.at[where],
                send_sem=row_sem,
                recv_sem=row_recv,
                device_id={"tp": 1 - side},
                device_id_type=mesh_id,
            )

        def edge_copy(to, where, slot):
            return pltpu.make_async_remote_copy(
                src_ref=x_ref.at[pl.ds(pl.multiple_of(side * (own_rows - HALO), HALO), HALO)],
                dst_ref=rows.at[pl.ds(where, HALO)],
                send_sem=edge_send.at[to],
                recv_sem=edge_recv.at[slot],
                device_id={"sp": (me + n + 2 * side - 1) % n, "tp": to},
                device_id_type=mesh_id,
            )

        edge_at = pl.multiple_of((1 - side) * (full - HALO), HALO)
        row_copy(place).start()
        for to in range(2):
            edge_copy(to, edge_at, side).start()

        def rows_ready():
            mine.wait()
            row_copy(other_place).wait_recv()
            edge_copy(0, 0, 1).wait_recv()
            edge_copy(0, full - HALO, 0).wait_recv()
            first = jnp.where(me == 0, 0.0, 1.0).astype(BF16)
            final = jnp.where(me == n - 1, 0.0, 1.0).astype(BF16)
            rows[pl.ds(0, HALO), :] = rows[pl.ds(0, HALO), :] * first
            rows[pl.ds(full - HALO, HALO), :] = rows[pl.ds(full - HALO, HALO), :] * final
            rows_ref[...] = rows[...]
    else:
        mine = pltpu.make_async_copy(x_ref, rows, own_sem.at[1])
        mine.start()

        def rows_ready():
            mine.wait()
            rows_ref[...] = rows[...]

    def multiply(step, way, first):
        for chunk in range(CHUNKS):
            mate_copy(step, way, chunk, True).wait_recv()
        where = chip_at(spot - step if way == 0 else spot + step)
        start, size = spans[way]
        tile = next(t for t in (768, 512, 256, 128) if size % t == 0)
        if tp == 2:
            inner = pl.ds(pl.multiple_of(where * 2 * depth, 2 * depth), 2 * depth)

        @pl.loop(0, size // tile)
        def _(i):
            at = pl.ds(pl.multiple_of(start + i * tile, 128), tile)
            w = wbuf[pl.ds(2 * where, 2), :, at].reshape(2 * depth, tile)
            lhs = rows[:, inner] if tp == 2 else rows[where]
            product = jnp.dot(lhs, w, preferred_element_type=F32)
            if first:
                acc[:, at] = product
            else:
                acc[:, at] += product

    waiting = []
    for step in range(chips - 1):
        for way, chunk in parts:
            arrival(step, way, chunk).wait_recv()
            if step < chips - 2:
                ring_copy(step + 1, way, chunk).start()
            mate_copy(step + 1, way, chunk).start()
        if step == 0:
            own.wait()
            waiting = [0]
        else:
            if step == 1:
                rows_ready()
            for done in waiting:
                for way in range(2):
                    multiply(done, way, done == 0)
            waiting = []
        waiting.append(step + 1)
    for done in waiting:
        for way in range(2):
            multiply(done, way, False)

    tile = next(t for t in (768, 512, 384, 256, 128) if cols % t == 0)

    @pl.loop(0, cols // tile)
    def _(i):
        at = pl.ds(pl.multiple_of(i * tile, 128), tile)
        proj_ref[:, at] = acc[:, at].astype(BF16)

    for step in range(chips):
        for way, chunk in parts:
            if step < chips - 1:
                ring_copy(step, way, chunk).wait_send()
            mate_copy(step, way, chunk).wait_send()
    if tp == 2:
        row_copy(place).wait_send()
        for to in range(2):
            edge_copy(to, edge_at, side).wait_send()


def enter(block, x, full, tp):
    n = lax.axis_size("sp")
    chips = n // 2
    depth, cols = block.shape
    shape = (full, x.shape[1]) if tp == 2 else x.shape
    vmem = pl.BlockSpec(memory_space=pltpu.VMEM)
    dma = pltpu.SemaphoreType.DMA
    return pl.pallas_call(
        functools.partial(entry_kernel, n, tp),
        out_shape=[
            jax.ShapeDtypeStruct((full, cols), BF16),
            jax.ShapeDtypeStruct(shape, BF16),
        ],
        in_specs=[vmem, vmem],
        out_specs=[vmem, vmem],
        scratch_shapes=[
            pltpu.VMEM((n, depth, cols), BF16),
            pltpu.VMEM(shape, BF16),
            pltpu.VMEM((full, cols), F32),
            dma((2,)),
            dma((chips - 1, 2, CHUNKS)),
            dma((chips - 1, 2, CHUNKS)),
            dma((chips, 2, CHUNKS)),
            dma((chips, 2, CHUNKS)),
            dma,
            dma,
            dma((2,)),
            dma((2,)),
        ],
        compiler_params=pltpu.CompilerParams(
            collective_id=0, has_side_effects=True, vmem_limit_bytes=56 * 2**20
        ),
        cost_estimate=pl.CostEstimate(
            flops=0, bytes_accessed=n * depth * cols * 16, transcendentals=0
        ),
    )(block, x)


def taps_of(padded, table, length):
    full = padded.shape[0]
    half = table.shape[0] // 2
    total = None
    for k in range(table.shape[0]):
        moved = padded if k == half else pltpu.roll(padded, (half - k) % full, 0)
        term = moved[HALO : HALO + length] * table[k : k + 1].astype(F32)
        total = term if total is None else total + term
    return total


def silu(v):
    return v * jax.nn.sigmoid(v)


def mix_kernel(
    og_ref, ig_ref, va_ref, x_ref, b_ref, c_ref, ct_ref, xt_ref, bt_ref, rt_ref,
    col_ref, row_ref, yconv_ref, within_ref, reads_ref, state_ref,
):
    length = yconv_ref.shape[0]
    gated = (ig_ref[...].astype(F32) * va_ref[...].astype(F32)).astype(BF16).astype(F32)
    conv = taps_of(gated, ct_ref[...], length)
    yconv_ref[...] = (og_ref[pl.ds(HALO, length), :].astype(F32) * conv).astype(BF16)
    xs = silu(taps_of(x_ref[...].astype(F32), xt_ref[...], length)).astype(BF16)
    bs = silu(taps_of(b_ref[...].astype(F32), bt_ref[...], length)).astype(BF16)
    cs = silu(taps_of(c_ref[...].astype(F32), rt_ref[...], length)).astype(BF16)
    reads_ref[...] = cs
    cols = col_ref[0]
    rows = row_ref[0]
    t_at = lax.broadcasted_iota(jnp.int32, (length, length), 0)
    s_at = lax.broadcasted_iota(jnp.int32, (length, length), 1)
    outs, weighted = [], []
    for h in range(2):
        c_h = cs[:, h * STATE : (h + 1) * STATE]
        b_h = bs[:, h * STATE : (h + 1) * STATE]
        x_h = xs[:, h * HEAD_DIM : (h + 1) * HEAD_DIM]
        o = 4 * h
        scores = lax.dot_general(
            c_h, b_h, (((1,), (1,)), ((), ())), preferred_element_type=F32
        )
        gap = jnp.where(
            t_at >= s_at,
            cols[:, o + 2 : o + 3] - rows[o + 2 : o + 3],
            cols[:, o + 3 : o + 4] - rows[o + 3 : o + 4],
        )
        d_f, d_b = rows[o : o + 1], rows[o + 1 : o + 2]
        scale = jnp.where(t_at > s_at, d_f, jnp.where(t_at < s_at, d_b, d_f + d_b))
        w = (scores * jnp.exp(gap) * scale).astype(BF16)
        outs.append(jnp.dot(w, x_h, preferred_element_type=F32))
        x32 = x_h.astype(F32)
        end_f = jnp.exp(rows[o + 2 : o + 3, length - 1 : length] - cols[:, o + 2 : o + 3])
        end_b = jnp.exp(rows[o + 3 : o + 4, 0:1] - cols[:, o + 3 : o + 4])
        both = jnp.concatenate(
            [x32 * (end_f * cols[:, o : o + 1]), x32 * (end_b * cols[:, o + 1 : o + 2])], axis=1
        ).astype(BF16)
        state_ref[h * STATE : (h + 1) * STATE] = lax.dot_general(
            both, b_h, (((0,), (0,)), ((), ())), preferred_element_type=F32
        ).astype(BF16)
    within_ref[...] = jnp.concatenate(outs, axis=1)


def exchange_kernel(
    n, share, s_ref, l_ref, out_ref, got, logs, enter, s_out, s_in, l_out, l_in, e_out, e_in
):
    me = lax.axis_index("sp")
    barrier = pltpu.get_barrier_semaphore()
    for k in range(1, n):
        pl.semaphore_signal(
            barrier,
            inc=1,
            device_id={"sp": (me + k) % n},
            device_id_type=pl.DeviceIdType.MESH,
        )
    pl.semaphore_wait(barrier, n - 1)

    def copy(src, dst, out_sem, in_sem, k, there, slot):
        return pltpu.make_async_remote_copy(
            src_ref=src.at[there],
            dst_ref=dst.at[slot],
            send_sem=out_sem.at[k],
            recv_sem=in_sem.at[k],
            device_id={"sp": there},
            device_id_type=pl.DeviceIdType.MESH,
        )

    for k in range(1, n):
        there = (me + k) % n
        copy(s_ref, got, s_out, s_in, k, there, me).start()
        copy(l_ref, logs, l_out, l_in, k, there, me).start()
    got[me] = s_ref[me]
    logs[me] = l_ref[me]
    for k in range(1, n):
        here = (me + n - k) % n
        copy(s_ref, got, s_out, s_in, k, here, here).wait_recv()
        copy(l_ref, logs, l_out, l_in, k, here, here).wait_recv()
    back = (me * share // HEAD_DIM) % 2
    acc = jnp.zeros(s_ref.shape[1:], F32)
    for i in range(n):
        j = back * (n - 1 - i) + (1 - back) * i
        enter[j] = acc.astype(BF16)
        acc = acc * jnp.exp(logs[j][0:1, :]) + got[j].astype(F32)
    out_ref[me] = enter[me]
    for k in range(1, n):
        copy(enter, out_ref, e_out, e_in, k, (me + k) % n, me).start()
    for k in range(1, n):
        here = (me + n - k) % n
        copy(enter, out_ref, e_out, e_in, k, here, here).wait_recv()
    for k in range(1, n):
        there = (me + k) % n
        copy(s_ref, got, s_out, s_in, k, there, me).wait_send()
        copy(l_ref, logs, l_out, l_in, k, there, me).wait_send()
        copy(enter, out_ref, e_out, e_in, k, there, me).wait_send()


def exchange_states(states, span_log):
    n, share, _ = states.shape
    assert HEAD_DIM % share == 0
    tables = jnp.repeat(span_log.reshape(-1), HEAD_DIM // share)
    tables = jnp.broadcast_to(tables[:, None, None], (n, 8, STATE))
    return pl.pallas_call(
        functools.partial(exchange_kernel, n, share),
        out_shape=jax.ShapeDtypeStruct(states.shape, BF16),
        in_specs=[pl.BlockSpec(memory_space=pltpu.VMEM)] * 2,
        out_specs=pl.BlockSpec(memory_space=pltpu.VMEM),
        scratch_shapes=[
            pltpu.VMEM(states.shape, BF16),
            pltpu.VMEM(tables.shape, F32),
            pltpu.VMEM(states.shape, BF16),
        ]
        + [pltpu.SemaphoreType.DMA((n,))] * 6,
        compiler_params=pltpu.CompilerParams(collective_id=1, has_side_effects=True),
        cost_estimate=pl.CostEstimate(flops=0, bytes_accessed=2**25, transcendentals=0),
    )(states, tables)


def finish_kernel(within_ref, reads_ref, enter_ref, gate_ref, gain_ref, col_ref, y_ref):
    length = y_ref.shape[0]
    cols = col_ref[0]
    outs = []
    for h in range(2):
        o = 4 * h
        both = lax.dot_general(
            reads_ref[:, h * STATE : (h + 1) * STATE],
            enter_ref[h * STATE : (h + 1) * STATE],
            (((1,), (1,)), ((), ())),
            preferred_element_type=F32,
        )
        here = slice(h * HEAD_DIM, (h + 1) * HEAD_DIM)
        y = within_ref[:, here]
        y = y + both[:, :HEAD_DIM] * jnp.exp(cols[:, o + 2 : o + 3])
        y = y + both[:, HEAD_DIM:] * jnp.exp(cols[:, o + 3 : o + 4])
        g = y * silu(gate_ref[pl.ds(HALO, length), :].astype(F32)[:, here])
        g = g * lax.rsqrt(jnp.mean(g * g, axis=-1, keepdims=True) + epsilon)
        outs.append(g * gain_ref[:, here].astype(F32))
    y_ref[...] = jnp.concatenate(outs, axis=1).astype(BF16)


def local(
    layer_source_rows, entry_rescale_factor, sliding_mixer_entry_matrix,
    recurrent_mixer_entry_matrix, latent_write_read_matrix, timestep_matrix,
    sliding_kernel_coefficients, recurrent_kernel_coefficients, latent_kernel_coefficients,
    lane_forgetting_rate, spike_forgetting_rate, lane_rescale_factor,
    sliding_mixer_exit_matrix, recurrent_mixer_exit_matrix,
):
    n = lax.axis_size("sp")
    tp = lax.axis_size("tp")
    own_rows, width = layer_source_rows.shape
    length = own_rows * tp
    full = length + 2 * HALO
    conv_width = sliding_mixer_entry_matrix.shape[2]
    ssd_width = recurrent_mixer_entry_matrix.shape[2]
    state_width = latent_write_read_matrix.shape[2]
    heads = timestep_matrix.shape[2]
    pairs = heads // 2
    cw = conv_width // pairs

    block = jnp.concatenate(
        [sliding_mixer_entry_matrix[i] for i in range(3)]
        + [recurrent_mixer_entry_matrix[i] for i in range(2)]
        + [latent_write_read_matrix[i] for i in range(2)],
        axis=1,
    )

    x32 = layer_source_rows.astype(F32)
    normed = (
        x32
        * lax.rsqrt(jnp.mean(x32 * x32, axis=-1, keepdims=True) + epsilon)
        * entry_rescale_factor.astype(F32)
    ).astype(BF16)
    if tp == 2:
        proj, rows = enter(block, normed, full, tp)
    else:
        up = [(i, i + 1) for i in range(n - 1)]
        down = [(i + 1, i) for i in range(n - 1)]
        shared = lax.all_gather(normed, "tp", axis=0, tiled=True)
        before = lax.ppermute(shared[length - HALO :], "sp", up)
        after = lax.ppermute(shared[:HALO], "sp", down)
        rows = jnp.concatenate([before, shared, after], axis=0)
        slabs = rows.reshape(full, n // 2, 2 * block.shape[0]).transpose(1, 0, 2)
        proj, _ = enter(block, slabs, full, tp)

    step_weight = timestep_matrix.reshape(width, 2 * heads)
    raw = jnp.dot(rows, step_weight, preferred_element_type=F32).astype(BF16)
    raw = raw[HALO : HALO + length].astype(F32).reshape(length, 2, heads)
    deltas = jax.nn.softplus(raw)
    logs = -deltas * lane_forgetting_rate[None] + spike_forgetting_rate[:, None, :]
    tri = (jnp.arange(length)[:, None] >= jnp.arange(length)[None, :]).astype(F32)
    run_f = jnp.dot(tri, logs[:, 0], precision=HIGHEST)
    run_b = jnp.dot(tri.T, logs[:, 1], precision=HIGHEST)
    table = jnp.stack([deltas[:, 0], deltas[:, 1], run_f, run_b], axis=2)
    col_table = table.reshape(length, pairs, 8).transpose(1, 0, 2)
    row_table = table.reshape(length, pairs, 8).transpose(1, 2, 0)
    span_log = jnp.stack([run_f[length - 1], run_b[0]], axis=1)
    share = heads * 2 * HEAD_DIM // n

    exit_c, proj = lax.optimization_barrier((sliding_mixer_exit_matrix, proj))
    exit_c = lax.all_gather(exit_c, "sp", axis=1, tiled=True)
    exit_s = lax.all_gather(recurrent_mixer_exit_matrix, "sp", axis=1, tiled=True)

    latent = latent_kernel_coefficients
    pw, sw = 2 * HEAD_DIM, 2 * STATE
    g0 = 3 * conv_width
    at_gate, at_x = g0 // pw, (g0 + ssd_width) // pw
    at_b = (g0 + 2 * ssd_width) // sw
    at_c = at_b + pairs
    y_conv, within, reads, states = pl.pallas_call(
        mix_kernel,
        grid=(pairs,),
        in_specs=[
            pl.BlockSpec((full, cw), lambda j: (0, j)),
            pl.BlockSpec((full, cw), lambda j: (0, pairs + j)),
            pl.BlockSpec((full, cw), lambda j: (0, 2 * pairs + j)),
            pl.BlockSpec((full, pw), lambda j: (0, at_x + j)),
            pl.BlockSpec((full, sw), lambda j: (0, at_b + j)),
            pl.BlockSpec((full, sw), lambda j: (0, at_c + j)),
            pl.BlockSpec((3, cw), lambda j: (0, j)),
            pl.BlockSpec((5, pw), lambda j: (0, j)),
            pl.BlockSpec((5, sw), lambda j: (0, j)),
            pl.BlockSpec((5, sw), lambda j: (0, pairs + j)),
            pl.BlockSpec((1, length, 8), lambda j: (j, 0, 0)),
            pl.BlockSpec((1, 8, length), lambda j: (j, 0, 0)),
        ],
        out_specs=[
            pl.BlockSpec((length, cw), lambda j: (0, j)),
            pl.BlockSpec((length, pw), lambda j: (0, j)),
            pl.BlockSpec((length, sw), lambda j: (0, j)),
            pl.BlockSpec((sw, STATE), lambda j: (j, 0)),
        ],
        out_shape=[
            jax.ShapeDtypeStruct((length, conv_width), BF16),
            jax.ShapeDtypeStruct((length, ssd_width), F32),
            jax.ShapeDtypeStruct((length, state_width), BF16),
            jax.ShapeDtypeStruct((pairs * sw, STATE), BF16),
        ],
        cost_estimate=pl.CostEstimate(
            flops=8 * length * length * heads * STATE, bytes_accessed=2**24, transcendentals=0
        ),
    )(
        proj, proj, proj, proj, proj, proj,
        sliding_kernel_coefficients, recurrent_kernel_coefficients,
        latent.reshape(latent.shape[0], -1), latent.reshape(latent.shape[0], -1),
        col_table, row_table,
    )

    entering = exchange_states(states.reshape(n, share, STATE), span_log)
    entering = entering.reshape(pairs * sw, STATE)

    y_ssd = pl.pallas_call(
        finish_kernel,
        grid=(pairs,),
        in_specs=[
            pl.BlockSpec((length, pw), lambda j: (0, j)),
            pl.BlockSpec((length, sw), lambda j: (0, j)),
            pl.BlockSpec((sw, STATE), lambda j: (j, 0)),
            pl.BlockSpec((full, pw), lambda j: (0, at_gate + j)),
            pl.BlockSpec((1, pw), lambda j: (0, j)),
            pl.BlockSpec((1, length, 8), lambda j: (j, 0, 0)),
        ],
        out_specs=pl.BlockSpec((length, pw), lambda j: (0, j)),
        out_shape=jax.ShapeDtypeStruct((length, ssd_width), BF16),
    )(within, reads, entering, proj, lane_rescale_factor.reshape(1, -1), col_table)

    def partial(y_c, y_s):
        return (
            jnp.dot(y_c, exit_c, preferred_element_type=F32)
            + jnp.dot(y_s, exit_s, preferred_element_type=F32)
        ).astype(BF16)

    if tp != 2:
        return lax.psum_scatter(
            partial(y_conv, y_ssd), "tp", scatter_dimension=0, tiled=True
        )
    tp_me = lax.axis_index("tp")

    def rows_of(owner, y):
        return lax.dynamic_slice_in_dim(y, owner * own_rows, own_rows, axis=0)

    away = partial(rows_of(1 - tp_me, y_conv), rows_of(1 - tp_me, y_ssd))
    arrived = lax.ppermute(away, "tp", [(0, 1), (1, 0)])
    kept = partial(rows_of(tp_me, y_conv), rows_of(tp_me, y_ssd))
    return (kept.astype(F32) + arrived.astype(F32)).astype(BF16)


def solution(mesh):
    placed = (
        P(("sp", "tp"), None),
        P(),
        P(None, "sp", "tp"),
        P(None, "sp", "tp"),
        P(None, "sp", "tp"),
        P(None, None, "tp"),
        P(None, "tp"),
        P(None, "tp"),
        P(None, None, "tp"),
        P(None, "tp"),
        P("sp", "tp"),
        P("tp"),
        P("tp", "sp"),
        P("tp", "sp"),
    )
    return jax.shard_map(
        local, mesh=mesh, in_specs=placed, out_specs=P(("sp", "tp"), None), check_vma=False
    )
```
